32 devices in a mesh: rep: 2 (over x), fs: 8 (over z, y), tp: 2 (over core).
Axes of the slice: x: 2, y: 2, z: 4, core: 2. Of those that a mesh axis runs over, the one named last changes fastest.
Arguments:
- tokens: bfloat16 [12288, 2048], P(('rep', 'fs'), 'tp'), may hold values from -6 to 6
- first_norm_gain: bfloat16 [2048], replicated, may hold values from 0.099609375 to 1.8984375
- query_projection_weight: bfloat16 [2048, 512], P('fs', 'tp'), may hold values from -0.125 to 0.125
- key_projection_weight: bfloat16 [2048, 512], P('fs', 'tp'), may hold values from -0.125 to 0.125
- value_projection_weight: bfloat16 [2048, 1024], P('fs', 'tp'), may hold values from -0.125 to 0.125
- output_gate_weight: bfloat16 [2048, 1024], P('fs', 'tp'), may hold values from -0.125 to 0.125
- decay_projection_weight: bfloat16 [2048, 512], P('fs', 'tp'), may hold values from -0.375 to 0.375
- fading_shift_vector: float32 [512], P('tp'), may hold values from -1 to 4
- added_fading_exponent: float32 [12288, 512], P(('rep', 'fs'), 'tp'), may hold values from -0.7 to 0
- per_head_gain: bfloat16 [128], replicated, may hold values from 0.099609375 to 1.8984375
- mixer_result_matrix: bfloat16 [1024, 2048], P('tp', 'fs'), may hold values from -0.1875 to 0.1875
- second_norm_gain: bfloat16 [2048], replicated, may hold values from 0.099609375 to 1.8984375
- up_linear_weight: bfloat16 [2048, 3072], P('fs', 'tp'), may hold values from -0.125 to 0.125
- up_gating_weight: bfloat16 [2048, 3072], P('fs', 'tp'), may hold values from -0.125 to 0.125
- depthwise_taps: bfloat16 [2, 3, 3072], P(None, None, 'tp'), may hold values from -3.5 to 3.5
- depthwise_bias: bfloat16 [2, 3072], P(None, 'tp'), may hold values from -3 to 3
- down_projection_weight: bfloat16 [3072, 2048], P('tp', 'fs'), may hold values from -0.109375 to 0.109375
Outputs:
- mixed: bfloat16 [12288, 2048], P(('rep', 'fs'), 'tp')
The draws below stay inside these ranges and needn't reach their ends.
All inputs are finite; a program needn't handle non-finite values.
Results may differ from the reference program's by a relative error of at most 0.018.
Values may be sent and summed in bfloat16 or wider, within the bound.
A program may use at most 128 MiB of HBM per device.

```python
import math
import jax
import jax.numpy as jnp
from jax import lax

D = 2048
HEADS = 8
KEY_DIM = 64
VALUE_DIM = 128
FF = 3072
KERNEL = 3
BLOCK = 64
SEQ_LEN = 256
TOKENS = 12288
N_TP = 2


def draw_added_fading_exponent(key, part):
    place_key, level_key = jax.random.split(jax.random.fold_in(key, 7))
    struck = jax.random.randint(place_key, (TOKENS, 1), 0, 64) == 0
    strength = jax.random.uniform(level_key, (TOKENS, HEADS * KEY_DIM), jnp.float32, math.log(0.5), math.log(0.8))
    return jnp.where(struck, strength, 0.0).astype(jnp.float32)


def levels(own_key, extent, pieces, smallest, largest):
    def one(dim, blocks):
        steps = jax.random.uniform(jax.random.fold_in(jax.random.fold_in(own_key, 6), dim), (blocks,), jnp.float32, smallest / len(pieces), largest / len(pieces))
        return jnp.repeat(jnp.exp(steps), extent[dim] // blocks).reshape((-1,) + (1,) * (len(extent) - dim - 1))

    level = one(*pieces[0])
    for cut in pieces[1:]:
        level = level * one(*cut)
    return level


def noise(stream_key, extent, deviation, most, cuts=(), kind=jnp.bfloat16):
    factor_of = levels(stream_key, extent, cuts, -0.22, 0.18) if cuts else 1.0
    drawn = jax.random.normal(stream_key, extent, jnp.float32) * deviation * factor_of
    return jnp.minimum(jnp.maximum(drawn, -most), most).astype(kind)


def setup_inputs(seed: int = 0) -> dict:
    key_list = jax.random.split(jax.random.key(seed), 18)
    tokens = noise(key_list[0], (TOKENS, D), 1.0, 6.0, ((0, 16), (1, 2)))
    first_norm_gain = jnp.clip(1.0 + 0.18 * jax.random.normal(key_list[1], (D,), jnp.float32), 0.099609375, 1.8984375).astype(jnp.bfloat16)
    query_projection_weight = noise(key_list[2], (D, HEADS * KEY_DIM), D ** -0.5, 0.125, ((0, 8), (1, 2)))
    key_projection_weight = noise(key_list[3], (D, HEADS * KEY_DIM), D ** -0.5, 0.125, ((0, 8), (1, 2)))
    value_projection_weight = noise(key_list[4], (D, HEADS * VALUE_DIM), D ** -0.5, 0.125, ((0, 8), (1, 2)))
    output_gate_weight = noise(key_list[5], (D, HEADS * VALUE_DIM), D ** -0.5, 0.125, ((0, 8), (1, 2)))
    decay_projection_weight = noise(key_list[6], (D, HEADS * KEY_DIM), (D // 9) ** -0.5, 0.375, ((0, 8), (1, 2)))
    fading_shift_vector = jnp.clip(-1.0 + 5.0 * jax.random.uniform(key_list[7], (HEADS * KEY_DIM,), jnp.float32) ** levels(key_list[7], (HEADS * KEY_DIM,), ((0, 2),), -0.2, 0.2), -1.0, 4.0)
    added_fading_exponent = draw_added_fading_exponent(jax.random.fold_in(key_list[17], 71), 0)
    per_head_gain = jnp.clip(1.0 + 0.18 * jax.random.normal(key_list[9], (VALUE_DIM,), jnp.float32), 0.099609375, 1.8984375).astype(jnp.bfloat16)
    mixer_result_matrix = noise(key_list[10], (HEADS * VALUE_DIM, D), (HEADS * VALUE_DIM) ** -0.5, 0.1875, ((0, 2), (1, 8)))
    second_norm_gain = jnp.clip(1.0 + 0.18 * jax.random.normal(key_list[11], (D,), jnp.float32), 0.099609375, 1.8984375).astype(jnp.bfloat16)
    up_linear_weight = noise(key_list[12], (D, FF), D ** -0.5, 0.125, ((0, 8), (1, 2)))
    up_gating_weight = noise(key_list[13], (D, FF), D ** -0.5, 0.125, ((0, 8), (1, 2)))
    depthwise_taps = noise(key_list[14], (2, KERNEL, FF), KERNEL ** -0.5, 3.5, ((2, 2),))
    depthwise_bias = noise(key_list[15], (2, FF), 0.5, 3.0, ((1, 2),))
    down_projection_weight = noise(key_list[16], (FF, D), FF ** -0.5, 0.109375, ((0, 2), (1, 8)))
    return dict(tokens=tokens, first_norm_gain=first_norm_gain, query_projection_weight=query_projection_weight, key_projection_weight=key_projection_weight, value_projection_weight=value_projection_weight, output_gate_weight=output_gate_weight, decay_projection_weight=decay_projection_weight, fading_shift_vector=fading_shift_vector, added_fading_exponent=added_fading_exponent, per_head_gain=per_head_gain, mixer_result_matrix=mixer_result_matrix, second_norm_gain=second_norm_gain, up_linear_weight=up_linear_weight, up_gating_weight=up_gating_weight, depthwise_taps=depthwise_taps, depthwise_bias=depthwise_bias, down_projection_weight=down_projection_weight)


norm_eps = 1e-06
fading_sharpness = 16.0

def normalize(source, gain):
    widened = source.astype(jnp.float32)
    scaled = widened * lax.rsqrt(lax.optimization_barrier(jnp.mean(widened * widened, axis=-1, keepdims=True)) + norm_eps)
    return (scaled * gain.astype(jnp.float32)).astype(jnp.bfloat16)

def direction(queries, key_heads, value_heads, fading_exponent):
    sequences, length, head_count, key_depth = queries.shape
    value_depth = value_heads.shape[-1]
    block_count = length // BLOCK
    query_blocks = queries.reshape(sequences, block_count, BLOCK, head_count, key_depth)
    key_blocks = key_heads.reshape(sequences, block_count, BLOCK, head_count, key_depth)
    value_blocks = value_heads.reshape(sequences, block_count, BLOCK, head_count, value_depth)
    cumulative = jnp.cumsum(fading_exponent.reshape(sequences, block_count, BLOCK, head_count, key_depth), axis=2)
    block_total = cumulative[:, :, -1:]
    query_decayed = query_blocks * jnp.exp(cumulative)
    key_inverse = key_blocks * jnp.exp(-cumulative)
    key_carried = key_blocks * jnp.exp(block_total - cumulative)
    lower_mask = jnp.tril(jnp.ones((BLOCK, BLOCK), dtype=bool))
    scores = jnp.einsum('snihd,snjhd->snhij', query_decayed, key_inverse, precision=lax.Precision.HIGHEST)
    scores = jnp.where(lower_mask, scores, 0.0)
    within_block = jnp.einsum('snhij,snjhv->snihv', scores, value_blocks, precision=lax.Precision.HIGHEST)
    increments = jnp.einsum('snchd,snchv->nshdv', key_carried, value_blocks, precision=lax.Precision.HIGHEST)
    carry_decay = jnp.moveaxis(jnp.exp(block_total[:, :, 0]), 1, 0)

    def advance(running, inputs):
        factor, update = inputs
        return (factor[..., None] * running + update, running)
    initial = jnp.zeros((sequences, head_count, key_depth, value_depth), jnp.float32)
    unused, previous = lax.scan(advance, initial, (carry_decay, increments))
    across_blocks = jnp.einsum('snchd,nshdv->snchv', query_decayed, previous, precision=lax.Precision.HIGHEST)
    return (within_block + across_blocks).reshape(sequences, length, head_count, value_depth)

def mixer_heads(queries_raw, keys_raw, values_raw, gates_raw, fading_exponent, per_head_gain):
    row_count = queries_raw.shape[0]
    head_count = values_raw.shape[1] // VALUE_DIM
    key_shape = (row_count // SEQ_LEN, SEQ_LEN, head_count, KEY_DIM)
    value_shape = (row_count // SEQ_LEN, SEQ_LEN, head_count, VALUE_DIM)
    queries = queries_raw.astype(jnp.float32).reshape(key_shape) * KEY_DIM ** (-0.5)
    key_heads = keys_raw.astype(jnp.float32).reshape(key_shape)
    value_heads = values_raw.astype(jnp.float32).reshape(value_shape)
    decay_heads = fading_exponent.reshape(key_shape)
    forward = direction(queries, key_heads, value_heads, decay_heads)
    backward = direction(jnp.flip(queries, 1), jnp.flip(key_heads, 1), jnp.flip(value_heads, 1), jnp.flip(decay_heads, 1))
    attention = forward + jnp.flip(backward, 1)
    scaled = attention * lax.rsqrt(lax.optimization_barrier(jnp.mean(attention * attention, axis=-1, keepdims=True)) + norm_eps)
    scaled = scaled * per_head_gain.astype(jnp.float32)
    merged = scaled.reshape(row_count, head_count * VALUE_DIM)
    return (merged * jax.nn.silu(gates_raw.astype(jnp.float32))).astype(jnp.bfloat16)

def depthwise(linear_out, gated_out, depthwise_taps, depthwise_bias):
    row_count, channels = linear_out.shape

    def smooth(source, taps, offset_bias):
        framed = source.astype(jnp.float32).reshape(row_count // SEQ_LEN, SEQ_LEN, channels)
        tap_count = taps.shape[0]
        leading_zero_fill = tap_count // 2
        padded = jnp.pad(framed, ((0, 0), (leading_zero_fill, tap_count - 1 - leading_zero_fill), (0, 0)))
        result = offset_bias.astype(jnp.float32)
        for shift_index in range(tap_count):
            result = result + padded[:, shift_index:shift_index + SEQ_LEN] * taps[shift_index].astype(jnp.float32)
        return result
    linear_conv = smooth(linear_out, depthwise_taps[0], depthwise_bias[0])
    gate_conv = smooth(gated_out, depthwise_taps[1], depthwise_bias[1])
    return (linear_conv * jax.nn.silu(gate_conv)).astype(jnp.bfloat16).reshape(row_count, channels)

def group_sum(left_side, right_side):
    group_rows = left_side.shape[1] // N_TP
    summed = jnp.zeros((left_side.shape[0], right_side.shape[1]), jnp.float32)
    for member in range(N_TP):
        partial_prod = jnp.dot(left_side[:, member * group_rows:(member + 1) * group_rows], right_side[member * group_rows:(member + 1) * group_rows], preferred_element_type=jnp.float32)
        summed = summed + lax.optimization_barrier(partial_prod.astype(jnp.bfloat16)).astype(jnp.float32)
    return summed

def reference(tokens, first_norm_gain, query_projection_weight, key_projection_weight, value_projection_weight, output_gate_weight, decay_projection_weight, fading_shift_vector, added_fading_exponent, per_head_gain, mixer_result_matrix, second_norm_gain, up_linear_weight, up_gating_weight, depthwise_taps, depthwise_bias, down_projection_weight):
    normed = normalize(tokens, first_norm_gain)
    queries_raw = jnp.dot(normed, query_projection_weight, preferred_element_type=jnp.float32).astype(jnp.bfloat16)
    keys_raw = jnp.dot(normed, key_projection_weight, preferred_element_type=jnp.float32).astype(jnp.bfloat16)
    values_raw = jnp.dot(normed, value_projection_weight, preferred_element_type=jnp.float32).astype(jnp.bfloat16)
    gates_raw = jnp.dot(normed, output_gate_weight, preferred_element_type=jnp.float32).astype(jnp.bfloat16)
    fading_scores_raw = jnp.dot(normed, decay_projection_weight, preferred_element_type=jnp.float32)
    fading_exponent = jax.nn.log_sigmoid(fading_scores_raw + fading_shift_vector) / fading_sharpness + added_fading_exponent
    mixed_heads = mixer_heads(queries_raw, keys_raw, values_raw, gates_raw, fading_exponent, per_head_gain)
    mixer_out = group_sum(mixed_heads, mixer_result_matrix)
    after_mixer = (tokens.astype(jnp.float32) + mixer_out).astype(jnp.bfloat16)
    normed_two = normalize(after_mixer, second_norm_gain)
    linear_out = jnp.dot(normed_two, up_linear_weight, preferred_element_type=jnp.float32).astype(jnp.bfloat16)
    gated_out = jnp.dot(normed_two, up_gating_weight, preferred_element_type=jnp.float32).astype(jnp.bfloat16)
    hidden = depthwise(linear_out, gated_out, depthwise_taps, depthwise_bias)
    channel_out = group_sum(hidden, down_projection_weight)
    return (after_mixer.astype(jnp.float32) + channel_out).astype(jnp.bfloat16)
```

```python
import functools
import jax
import jax.numpy as jnp
from jax import lax
from jax.experimental import pallas as pl
from jax.experimental.pallas import tpu as pltpu
from jax.sharding import PartitionSpec as P

KEY_DIM = 64
VALUE_DIM = 128
BLOCK = 64
SEQ_LEN = 256
CHUNK = 256

norm_eps = 1e-06
fading_sharpness = 16.0
F32 = jnp.float32
BF16 = jnp.bfloat16


class Gather:
    def __init__(self, n, shared, own, full, recv, send):
        self.n, self.outer, self.shared = n, n // 2, shared
        self.own, self.full, self.recv, self.send = own, full, recv, send
        self.rows = own.shape[0]
        self.rep = lax.axis_index("rep")
        self.me = lax.axis_index("fs")
        self.hi, self.lo = self.me // 2, lax.rem(self.me, 2)
        self.half = self.rep if shared else 0

    def piece(self, ref, shard, half):
        rows = self.rows // 2 if self.shared else self.rows
        base = half * rows if shard is None else shard * self.rows + half * rows
        return ref.at[pl.ds(pl.multiple_of(base, rows), rows)]

    def local(self, sem):
        span = pl.ds(pl.multiple_of(self.me * self.rows, self.rows), self.rows)
        return pltpu.make_async_copy(self.own, self.full.at[span], sem)

    def copy(self, shard, half, slot, target, own=False):
        there = self.piece(self.full, shard, half)
        return pltpu.make_async_remote_copy(
            src_ref=self.piece(self.own, None, half) if own else there,
            dst_ref=there,
            send_sem=self.send.at[slot],
            recv_sem=self.recv.at[shard, half],
            device_id=target,
            device_id_type=pl.DeviceIdType.MESH,
        )

    def pair(self):
        return {"fs": self.hi * 2 + 1 - self.lo}

    def other(self):
        return {"rep": 1 - self.rep}

    def back(self, d, lo):
        return lax.rem(self.hi - d + self.outer, self.outer) * 2 + lo

    def start_outer(self):
        for d in range(1, self.outer):
            target = lax.rem(self.hi + d, self.outer) * 2 + self.lo
            self.copy(self.me, self.half, d - 1, {"fs": target}, own=True).start()

    def start_pair(self):
        self.copy(self.me, self.half, self.outer - 1, self.pair(), own=True).start()

    def outer_event(self, d):
        shard = self.back(d, self.lo)
        self.copy(shard, self.half, 0, self.pair()).wait_recv()
        self.copy(shard, self.half, self.outer - 1 + d, self.pair()).start()
        if self.shared:
            self.copy(shard, self.half, 2 * self.outer - 1 + d - 1, self.other()).start()

    def pair_event(self, d):
        shard = self.back(d, 1 - self.lo)
        self.copy(shard, self.half, 0, self.pair()).wait_recv()
        if self.shared:
            self.copy(shard, self.half, 3 * self.outer - 2 + d, self.other()).start()

    def rep_events(self):
        if self.shared:
            for d in range(1, self.outer):
                self.copy(self.back(d, self.lo), 1 - self.half, 0, self.other()).wait_recv()
            for d in range(self.outer):
                self.copy(self.back(d, 1 - self.lo), 1 - self.half, 0, self.other()).wait_recv()

    def finish(self):
        for slot in range((4 if self.shared else 2) * self.outer - (2 if self.shared else 1)):
            self.copy(self.me, self.half, slot, self.pair()).wait_send()


def greet(n):
    me, rep = lax.axis_index("fs"), lax.axis_index("rep")
    hi, lo, outer = me // 2, lax.rem(me, 2), n // 2
    barrier = pltpu.get_barrier_semaphore()
    targets = [{"fs": lax.rem(hi + d, outer) * 2 + lo} for d in range(1, outer)]
    targets += [{"fs": hi * 2 + 1 - lo}, {"rep": 1 - rep}, {"tp": 1 - lax.axis_index("tp")}]
    for target in targets:
        pl.semaphore_signal(barrier, inc=1, device_id=target, device_id_type=pl.DeviceIdType.MESH)
    pl.semaphore_wait(barrier, len(targets))


SHARED = (True, False, True, False)


def matmul(left, right):
    return jnp.dot(left, right, preferred_element_type=F32)


def matmul_t(left, right):
    return lax.dot_general(left, right, (((1,), (1,)), ((), ())), preferred_element_type=F32)


def matmul_0(left, right):
    return lax.dot_general(left, right, (((0,), (0,)), ((), ())), preferred_element_type=F32)


def silu(x):
    return x / (1.0 + jnp.exp(-x))


def scaled_rows(x, gain):
    return (x * lax.rsqrt(jnp.mean(x * x, axis=-1, keepdims=True) + norm_eps) * gain).astype(BF16)


def attend(rows, proj, decay, mixed, head_gain, keys, values):
    blocks = SEQ_LEN // BLOCK
    row = lax.broadcasted_iota(jnp.int32, (SEQ_LEN, SEQ_LEN), 0)
    column = lax.broadcasted_iota(jnp.int32, (SEQ_LEN, SEQ_LEN), 1)
    tri = jnp.where((row >= column) & (row // BLOCK == column // BLOCK), 1.0, 0.0).astype(BF16)
    small_row = lax.broadcasted_iota(jnp.int32, (BLOCK, BLOCK), 0)
    small_column = lax.broadcasted_iota(jnp.int32, (BLOCK, BLOCK), 1)
    lane = lax.broadcasted_iota(jnp.int32, (1, 2 * KEY_DIM), 1)
    for pair in range(keys // (2 * KEY_DIM)):
        at = pair * 2 * KEY_DIM
        span = slice(at, at + 2 * KEY_DIM)
        ld = decay[rows, span]
        high = ld.astype(BF16)
        low = (ld - high.astype(F32)).astype(BF16)
        cum = matmul(tri, high) + matmul(tri, low)
        q = proj[rows, span].astype(F32) * KEY_DIM ** (-0.5)
        k = proj[rows, keys + at : keys + at + 2 * KEY_DIM].astype(F32)
        parts = []
        for b in range(blocks):
            inside = slice(b * BLOCK, (b + 1) * BLOCK)
            c, x, y = cum[inside], q[inside], k[inside]
            e = c - ld[inside]
            total = c[BLOCK - 1 : BLOCK]
            r = total - e
            parts.append(
                (
                    (x * jnp.exp(c)).astype(BF16),
                    y * jnp.exp(-c),
                    y * jnp.exp(total - c),
                    (x * jnp.exp(r)).astype(BF16),
                    y * jnp.exp(-r),
                    y * jnp.exp(e),
                    jnp.exp(total),
                )
            )
        for h in range(2):
            mask = (lane // KEY_DIM) == h

            def only(z):
                return jnp.where(mask, z, 0.0).astype(BF16)

            head = pair * 2 + h
            at_v = 2 * keys + head * VALUE_DIM
            v = proj[rows, at_v : at_v + VALUE_DIM]
            gate = proj[rows, at_v + values : at_v + values + VALUE_DIM].astype(F32)
            outs = []
            for b in range(blocks):
                qf, kf, _, qb, kb, _, _ = parts[b]
                scores = jnp.where(small_row >= small_column, matmul_t(qf, only(kf)), 0.0)
                scores += jnp.where(small_row <= small_column, matmul_t(qb, only(kb)), 0.0)
                outs.append(matmul(scores.astype(BF16), v[b * BLOCK : (b + 1) * BLOCK]))
            state = None
            for b in range(blocks):
                if state is not None:
                    outs[b] += matmul_t(parts[b][0], state.astype(BF16))
                if b < blocks - 1:
                    update = matmul_0(v[b * BLOCK : (b + 1) * BLOCK], only(parts[b][2]))
                    state = update if state is None else state * parts[b][6] + update
            state = None
            for b in reversed(range(blocks)):
                if state is not None:
                    outs[b] += matmul_t(parts[b][3], state.astype(BF16))
                if b > 0:
                    update = matmul_0(v[b * BLOCK : (b + 1) * BLOCK], only(parts[b][5]))
                    state = update if state is None else state * parts[b][6] + update
            y = jnp.concatenate(outs, axis=0)
            y = y * lax.rsqrt(jnp.mean(y * y, axis=-1, keepdims=True) + norm_eps) * head_gain
            mixed[rows, head * VALUE_DIM : (head + 1) * VALUE_DIM] = (y * silu(gate)).astype(BF16)


def layer_kernel(n, keys, values, *refs):
    tokens, added, shift, gain_one, gain_two, head_gain, conv = refs[:7]
    owns, out = refs[7:11], refs[11]
    fulls = refs[12:16]
    tok, normed, terms, theirs, proj, decay, mixed, arrived = refs[16:24]
    recvs, sends = refs[24:28], refs[28:32]
    local_sem, tp_send, tp_recv = refs[32:35]
    t = lax.axis_index("tp")
    count, share = tokens.shape
    units = conv.shape[1]
    mine = pl.ds(pl.multiple_of(t * share, share), share)
    greet(n)

    def swap(source, target, slot):
        return pltpu.make_async_remote_copy(
            src_ref=source,
            dst_ref=target,
            send_sem=tp_send.at[slot],
            recv_sem=tp_recv.at[slot],
            device_id={"tp": 1 - t},
            device_id_type=pl.DeviceIdType.MESH,
        )

    token_swap = swap(tokens, tok.at[:, mine], 0)
    token_swap.start()
    gathers = [Gather(n, *entry) for entry in zip(SHARED, owns, fulls, recvs, sends)]
    a, m, u, d = gathers
    outer = a.outer
    for g in gathers:
        g.start_outer()
    a.start_pair()
    m.start_pair()
    locals_ = [g.local(local_sem.at[i]) for i, g in enumerate(gathers)]
    locals_.append(pltpu.make_async_copy(tokens, tok.at[:, mine], local_sem.at[4]))
    for c in locals_:
        c.start()
    for c in locals_:
        c.wait()
    token_swap.wait()
    step = 64

    @pl.loop(0, count // step)
    def _(i):
        rows = pl.ds(pl.multiple_of(i * step, step), step)
        normed[rows] = scaled_rows(tok[rows].astype(F32), gain_one[...])

    def through(g, first, last):
        for k in range(first, last):
            g.outer_event(k)
            g.pair_event(k)

    a.pair_event(0)
    through(a, 1, outer)
    u.start_pair()
    m.pair_event(0)
    through(m, 1, outer)
    u.pair_event(0)
    a.rep_events()
    attention_full, mixer_full, up_full, down_full = fulls

    @pl.loop(0, (2 * keys + 2 * values) // CHUNK)
    def _(j):
        cols = pl.ds(pl.multiple_of(j * CHUNK, CHUNK), CHUNK)
        proj[:, cols] = matmul(normed[...], attention_full[:, cols]).astype(BF16)

    z = matmul(normed[...], attention_full[:, 2 * keys + 2 * values :]) + shift[...]
    log_sigmoid = jnp.minimum(z, 0.0) - jnp.log(1.0 + jnp.exp(-jnp.abs(z)))
    decay[...] = log_sigmoid / fading_sharpness + added[...]
    half = (outer + 1) // 2
    through(u, 1, half + 1)
    d.start_pair()

    @pl.loop(0, count // SEQ_LEN)
    def _(s):
        rows = pl.ds(pl.multiple_of(s * SEQ_LEN, SEQ_LEN), SEQ_LEN)
        attend(rows, proj, decay, mixed, head_gain[...], keys, values)

    through(u, half + 1, outer)
    d.pair_event(0)
    swaps = []
    for part in range(2):

        @pl.loop(0, share // CHUNK)
        def _(j):
            cols = pl.ds(pl.multiple_of(part * share + j * CHUNK, CHUNK), CHUNK)
            terms[:, cols] = matmul_t(mixed[...], mixer_full[cols]).astype(BF16)

        cols = pl.ds(part * share, share)
        swaps.append(swap(terms.at[:, cols], theirs.at[:, cols], 1 + part))
        swaps[-1].start()
    for c in swaps:
        c.wait()

    @pl.loop(0, count // step)
    def _(i):
        rows = pl.ds(pl.multiple_of(i * step, step), step)
        summed = terms[rows].astype(F32) + theirs[rows].astype(F32)
        after = (tok[rows].astype(F32) + summed).astype(BF16)
        tok[rows] = after
        normed[rows] = scaled_rows(after.astype(F32), gain_two[...])

    through(d, 1, outer - 1)
    u.rep_events()
    if outer > 1:
        d.outer_event(outer - 1)
    place = lax.rem(lax.broadcasted_iota(jnp.int32, (count, 1), 0), SEQ_LEN)

    def smooth(x, taps, bias):
        x = x.astype(BF16).astype(F32)
        before = jnp.where(place == 0, 0.0, pltpu.roll(x, 1, 0))
        behind = jnp.where(place == SEQ_LEN - 1, 0.0, pltpu.roll(x, count - 1, 0))
        return bias + before * taps[0:1] + x * taps[1:2] + behind * taps[2:3]

    @pl.loop(0, units // CHUNK)
    def _(j):
        cols = pl.ds(pl.multiple_of(j * CHUNK, CHUNK), CHUNK)
        gate_cols = pl.ds(pl.multiple_of(units + j * CHUNK, CHUNK), CHUNK)
        table = conv[:, cols]
        linear = smooth(matmul(normed[...], up_full[:, cols]), table[0:3], table[6:7])
        gate = smooth(matmul(normed[...], up_full[:, gate_cols]), table[3:6], table[7:8])
        proj[:, cols] = (linear * silu(gate)).astype(BF16)

    if outer > 1:
        d.pair_event(outer - 1)
    for part in range(2):
        base = lax.rem(t + 1 + part, 2) * share

        @pl.loop(0, share // CHUNK)
        def _(j):
            cols = pl.ds(pl.multiple_of(part * share + j * CHUNK, CHUNK), CHUNK)
            units_rows = pl.ds(pl.multiple_of(base + j * CHUNK, CHUNK), CHUNK)
            terms[:, cols] = matmul_t(proj[:, :units], down_full[units_rows]).astype(BF16)

        if part == 0:
            last = swap(terms.at[:, pl.ds(0, share)], arrived, 3)
            last.start()
    last.wait()

    @pl.loop(0, count // step)
    def _(i):
        rows = pl.ds(pl.multiple_of(i * step, step), step)
        summed = terms[rows, share:].astype(F32) + arrived[rows].astype(F32)
        out[rows] = (tok[rows, mine].astype(F32) + summed).astype(BF16)

    for g in gathers:
        g.finish()


def local(
    n,
    tokens,
    first_norm_gain,
    query_projection_weight,
    key_projection_weight,
    value_projection_weight,
    output_gate_weight,
    decay_projection_weight,
    fading_shift_vector,
    added_fading_exponent,
    per_head_gain,
    mixer_result_matrix,
    second_norm_gain,
    up_linear_weight,
    up_gating_weight,
    depthwise_taps,
    depthwise_bias,
    down_projection_weight,
):
    attention_weight = jnp.concatenate(
        [
            query_projection_weight,
            key_projection_weight,
            value_projection_weight,
            output_gate_weight,
            decay_projection_weight,
        ],
        axis=1,
    )
    up_weight = jnp.concatenate([up_linear_weight, up_gating_weight], axis=1)
    shards = (attention_weight, mixer_result_matrix.T, up_weight, down_projection_weight.T)
    keys, values = query_projection_weight.shape[1], value_projection_weight.shape[1]
    units = up_linear_weight.shape[1]
    conv = jnp.concatenate(
        [depthwise_taps.reshape(-1, units), depthwise_bias], axis=0
    ).astype(F32)
    count, share = tokens.shape
    wide = max(units, 2 * keys + 2 * values)
    outer = n // 2
    anywhere = pl.BlockSpec(memory_space=pl.ANY)
    vmem = pl.BlockSpec(memory_space=pltpu.VMEM)
    return pl.pallas_call(
        functools.partial(layer_kernel, n, keys, values),
        out_shape=jax.ShapeDtypeStruct(tokens.shape, BF16),
        in_specs=[anywhere] + [vmem] * 6 + [anywhere] * 4,
        out_specs=vmem,
        scratch_shapes=[pltpu.VMEM((n * s.shape[0], s.shape[1]), BF16) for s in shards]
        + [
            pltpu.VMEM((count, 2 * share), BF16),
            pltpu.VMEM((count, 2 * share), BF16),
            pltpu.VMEM((count, 2 * share), BF16),
            pltpu.VMEM((count, 2 * share), BF16),
            pltpu.VMEM((count, wide), BF16),
            pltpu.VMEM((count, keys), F32),
            pltpu.VMEM((count, values), BF16),
            pltpu.VMEM((count, share), BF16),
        ]
        + [pltpu.SemaphoreType.DMA((n, 2)) for s in shards]
        + [pltpu.SemaphoreType.DMA((4 * outer,)) for s in shards]
        + [
            pltpu.SemaphoreType.DMA((5,)),
            pltpu.SemaphoreType.DMA((4,)),
            pltpu.SemaphoreType.DMA((4,)),
        ],
        compiler_params=pltpu.CompilerParams(
            collective_id=0, has_side_effects=True, vmem_limit_bytes=67043328
        ),
        name="layer",
    )(
        tokens,
        added_fading_exponent,
        fading_shift_vector.reshape(1, -1),
        first_norm_gain.astype(F32).reshape(1, -1),
        second_norm_gain.astype(F32).reshape(1, -1),
        per_head_gain.astype(F32).reshape(1, -1),
        conv,
        *shards,
    )


def solution(mesh):
    return jax.shard_map(
        functools.partial(local, mesh.shape["fs"]),
        mesh=mesh,
        in_specs=(
            P(("rep", "fs"), "tp"),
            P(),
            P("fs", "tp"),
            P("fs", "tp"),
            P("fs", "tp"),
            P("fs", "tp"),
            P("fs", "tp"),
            P("tp"),
            P(("rep", "fs"), "tp"),
            P(),
            P("tp", "fs"),
            P(),
            P("fs", "tp"),
            P("fs", "tp"),
            P(None, None, "tp"),
            P(None, "tp"),
            P("tp", "fs"),
        ),
        out_specs=P(("rep", "fs"), "tp"),
        check_vma=False,
    )
```
